32 devices in a mesh: rep: 2 (over y), fs: 4 (over z), tp: 4 (over x, core).
Axes of the slice: x: 2, y: 2, z: 4, core: 2. Of those that a mesh axis runs over, the one named last changes fastest.
Arguments:
- stream: bfloat16 [2048, 1536], P(('rep', 'fs')), may hold values from -6 to 6
- mix_pre_gain: float32 [1536], replicated, may hold values from 0.1 to 1.9
- w_outer_gate: bfloat16 [1536, 768], P('fs', 'tp'), may hold values from -0.15625 to 0.15625
- w_inner_gate: bfloat16 [1536, 768], P('fs', 'tp'), may hold values from -0.15625 to 0.15625
- w_value: bfloat16 [1536, 768], P('fs', 'tp'), may hold values from -0.15625 to 0.15625
- mix_taps: float32 [3, 768], P(None, 'tp'), may hold values from -3 to 3
- w_mix_out: bfloat16 [768, 1536], P('tp', 'fs'), may hold values from -0.3125 to 0.3125
- mix_post_gain: float32 [1536], replicated, may hold values from 0.1 to 1.9
- ffn_pre_gain: float32 [1536], replicated, may hold values from 0.1 to 1.9
- w_linear: bfloat16 [1536, 4224], P('fs', 'tp'), may hold values from -0.15625 to 0.15625
- w_gated: bfloat16 [1536, 4224], P('fs', 'tp'), may hold values from -0.15625 to 0.15625
- ffn_taps: float32 [3, 4224], P(None, 'tp'), may hold values from -3 to 3
- ffn_bias: float32 [4224], P('tp'), may hold values from -3 to 3
- w_down: bfloat16 [4224, 1536], P('tp', 'fs'), may hold values from -0.125 to 0.125
- ffn_post_gain: float32 [1536], replicated, may hold values from 0.1 to 1.9
Outputs:
- result: bfloat16 [2048, 1536], P(('rep', 'fs'))
The draws below stay inside these ranges and needn't reach their ends.
All inputs are finite; a program needn't handle non-finite values.
Results may differ from the reference program's by a relative error of at most 0.023.
Values may be sent and summed in bfloat16 or wider, within the bound.
A program may use at most 64 MiB of HBM per device.

```python
import jax
import jax.numpy as jnp
from jax import lax

D = 1536
CONV_W = 768
FF = 4224
SEQ_LEN = 128
TOKENS = 2048
N_TP = 4


def spiked(entries, stream_key, source, target, blocks, factor):
    owner, partner = [(jnp.arange(entries.shape[position]) // (entries.shape[position] // blocks)).reshape([-1 if axis == position else 1 for axis in range(entries.ndim)]) for position in (source, target)]
    chosen = jax.random.permutation(stream_key, blocks)[partner]
    strong = (owner == chosen) | (owner == (partner + blocks // 2) % blocks)
    return jnp.where(strong, factor * entries, entries)


def block_levels(own_key, dims, shards, least, largest):
    factor_of, own = 1.0, jax.random.fold_in(own_key, 6)
    for axis_at, shards_of in shards:
        draws = jnp.exp(jax.random.uniform(jax.random.fold_in(own, axis_at), (shards_of,), jnp.float32, least / len(shards), largest / len(shards)))
        factor_of = factor_of * jnp.repeat(draws, dims[axis_at] // shards_of).reshape([-1 if axis == axis_at else 1 for axis in range(len(dims))])
    return factor_of


def scatter_about(stream_key, dims, deviation, limit, cuts=(), held_as=jnp.bfloat16):
    drawn = jax.random.normal(stream_key, dims, jnp.float32) * deviation
    if len(cuts) > 0:
        drawn = block_levels(stream_key, dims, cuts, -0.22, 0.18) * drawn
    return jnp.clip(drawn, min=-limit, max=limit).astype(held_as)


def gaussian_with(own_key, shape, scale, reach, shards, heavy, kind=jnp.bfloat16):
    values = scale * jax.random.normal(own_key, shape, jnp.float32)
    if shards:
        values = values * block_levels(own_key, shape, shards, -0.22, 0.18)
    return jnp.clip(spiked(values, jax.random.fold_in(own_key, 3), *heavy), -reach, reach).astype(kind)


def setup_inputs(seed: int = 0) -> dict:
    streams_of = jax.random.split(jax.random.key(seed), 16)
    stream = scatter_about(streams_of[0], (TOKENS, D), 1.0, 6.0, ((0, 8),))
    mix_pre_gain = jnp.clip(1.0 + 0.18 * jax.random.normal(streams_of[1], (D,), jnp.float32), 0.1, 1.9)
    w_outer_gate = scatter_about(streams_of[2], (D, CONV_W), D ** -0.5, 0.15625, ((0, 4), (1, 4)))
    w_inner_gate = scatter_about(streams_of[3], (D, CONV_W), D ** -0.5, 0.15625, ((0, 4), (1, 4)))
    w_value = scatter_about(streams_of[4], (D, CONV_W), D ** -0.5, 0.15625, ((0, 4), (1, 4)))
    mix_taps = scatter_about(streams_of[5], (3, CONV_W), 0.577, 3.0, ((1, 4),), jnp.float32)
    w_mix_out = gaussian_with(streams_of[6], (CONV_W, D), CONV_W ** -0.5, 0.3125, ((0, 4), (1, 4)), (0, 1, 4, 2.0))
    mix_post_gain = jnp.clip(1.0 + 0.18 * jax.random.normal(streams_of[7], (D,), jnp.float32), 0.1, 1.9)
    ffn_pre_gain = jnp.clip(1.0 + 0.18 * jax.random.normal(streams_of[8], (D,), jnp.float32), 0.1, 1.9)
    w_linear = scatter_about(streams_of[9], (D, FF), D ** -0.5, 0.15625, ((0, 4), (1, 4)))
    w_gated = scatter_about(streams_of[10], (D, FF), D ** -0.5, 0.15625, ((0, 4), (1, 4)))
    ffn_taps = scatter_about(streams_of[11], (3, FF), 0.577, 3.0, ((1, 4),), jnp.float32)
    ffn_bias = scatter_about(streams_of[12], (FF,), 0.5, 3.0, ((0, 4),), jnp.float32)
    w_down = gaussian_with(streams_of[13], (FF, D), FF ** -0.5, 0.125, ((0, 4), (1, 4)), (0, 1, 4, 2.0))
    ffn_post_gain = jnp.clip(1.0 + 0.18 * jax.random.normal(streams_of[14], (D,), jnp.float32), 0.1, 1.9)
    return {"stream": stream, "mix_pre_gain": mix_pre_gain, "w_outer_gate": w_outer_gate, "w_inner_gate": w_inner_gate, "w_value": w_value, "mix_taps": mix_taps, "w_mix_out": w_mix_out, "mix_post_gain": mix_post_gain, "ffn_pre_gain": ffn_pre_gain, "w_linear": w_linear, "w_gated": w_gated, "ffn_taps": ffn_taps, "ffn_bias": ffn_bias, "w_down": w_down, "ffn_post_gain": ffn_post_gain}


EPS = 1e-06

def norm_scale(values, gain):
    return values * lax.rsqrt(lax.optimization_barrier(jnp.mean(values * values, axis=-1, keepdims=True)) + EPS) * gain

def conv_three(values, taps):
    height, breadth = values.shape
    grouped = values.reshape(height // SEQ_LEN, SEQ_LEN, breadth)
    padded = jnp.pad(grouped, ((0, 0), (1, 1), (0, 0)))
    mixed = taps[0] * padded[:, :-2] + taps[1] * padded[:, 1:-1] + taps[2] * padded[:, 2:]
    return mixed.reshape(height, breadth)

def blocked_sum(left, right):
    block_cols = left.shape[1] // N_TP
    summed = jnp.zeros((left.shape[0], right.shape[1]), jnp.float32)
    for block in range(N_TP):
        partial_value = jnp.dot(left[:, block * block_cols:(block + 1) * block_cols], right[block * block_cols:(block + 1) * block_cols], preferred_element_type=jnp.float32)
        rounded = lax.optimization_barrier(partial_value.astype(jnp.bfloat16))
        summed = summed + rounded.astype(jnp.float32)
    return summed.astype(jnp.bfloat16)

def reference(stream, mix_pre_gain, w_outer_gate, w_inner_gate, w_value, mix_taps, w_mix_out, mix_post_gain, ffn_pre_gain, w_linear, w_gated, ffn_taps, ffn_bias, w_down, ffn_post_gain):
    resid = stream.astype(jnp.float32)
    normed = norm_scale(resid, mix_pre_gain).astype(jnp.bfloat16)
    outer = jnp.dot(normed, w_outer_gate, preferred_element_type=jnp.float32).astype(jnp.bfloat16)
    inner = jnp.dot(normed, w_inner_gate, preferred_element_type=jnp.float32).astype(jnp.bfloat16)
    value = jnp.dot(normed, w_value, preferred_element_type=jnp.float32).astype(jnp.bfloat16)
    product = inner.astype(jnp.float32) * value.astype(jnp.float32)
    mixed = (outer.astype(jnp.float32) * conv_three(product, mix_taps)).astype(jnp.bfloat16)
    branch = blocked_sum(mixed, w_mix_out)
    middle = (resid + norm_scale(branch.astype(jnp.float32), mix_post_gain)).astype(jnp.bfloat16)
    middle_f = middle.astype(jnp.float32)
    normed_two = norm_scale(middle_f, ffn_pre_gain).astype(jnp.bfloat16)
    linear = jnp.dot(normed_two, w_linear, preferred_element_type=jnp.float32).astype(jnp.bfloat16)
    gated = jnp.dot(normed_two, w_gated, preferred_element_type=jnp.float32).astype(jnp.bfloat16)
    activated = jax.nn.gelu(conv_three(gated.astype(jnp.float32), ffn_taps) + ffn_bias, approximate=True)
    hidden = (activated * linear.astype(jnp.float32)).astype(jnp.bfloat16)
    branch_two = blocked_sum(hidden, w_down)
    return (middle_f + norm_scale(branch_two.astype(jnp.float32), ffn_post_gain)).astype(jnp.bfloat16)
```

```python
import functools

import jax
import jax.numpy as jnp
from jax import lax
from jax.experimental import pallas as pl
from jax.experimental.pallas import tpu as pltpu
from jax.sharding import PartitionSpec as P

SEQ_LEN = 128
PACK = 16


EPS = 1e-06


def norm_scale(values, gain):
    return values * lax.rsqrt(jnp.mean(values * values, axis=-1, keepdims=True) + EPS) * gain


def conv_three(values, taps):
    height, breadth = values.shape
    grouped = values.reshape(height // SEQ_LEN, SEQ_LEN, breadth)
    padded = jnp.pad(grouped, ((0, 0), (1, 1), (0, 0)))
    mixed = taps[0] * padded[:, :-2] + taps[1] * padded[:, 1:-1] + taps[2] * padded[:, 2:]
    return mixed.reshape(height, breadth)


def settle(partial_value, resid, post_gain):
    branch = lax.psum(partial_value.astype(jnp.bfloat16), "tp")
    return (resid + norm_scale(branch.astype(jnp.float32), post_gain)).astype(jnp.bfloat16)


def gather_plan(
    stream,
    mix_pre_gain,
    w_outer_gate,
    w_inner_gate,
    w_value,
    mix_taps,
    w_mix_out,
    mix_post_gain,
    ffn_pre_gain,
    w_linear,
    w_gated,
    ffn_taps,
    ffn_bias,
    w_down,
    ffn_post_gain,
):
    resid = stream.astype(jnp.float32)
    normed = norm_scale(resid, mix_pre_gain).astype(jnp.bfloat16)
    full_outer, full_inner, full_value = (
        lax.all_gather(w_outer_gate, "fs", axis=0, tiled=True),
        lax.all_gather(w_inner_gate, "fs", axis=0, tiled=True),
        lax.all_gather(w_value, "fs", axis=0, tiled=True),
    )
    outer = jnp.dot(normed, full_outer, preferred_element_type=jnp.float32)
    inner = jnp.dot(normed, full_inner, preferred_element_type=jnp.float32)
    value = jnp.dot(normed, full_value, preferred_element_type=jnp.float32)
    outer = outer.astype(jnp.bfloat16)
    inner = inner.astype(jnp.bfloat16)
    value = value.astype(jnp.bfloat16)
    product = inner.astype(jnp.float32) * value.astype(jnp.float32)
    mixed = (outer.astype(jnp.float32) * conv_three(product, mix_taps)).astype(jnp.bfloat16)
    full_mix_out = lax.all_gather(w_mix_out, "fs", axis=1, tiled=True)
    partial_value = jnp.dot(mixed, full_mix_out, preferred_element_type=jnp.float32)
    middle = settle(partial_value, resid, mix_post_gain)
    middle_f = middle.astype(jnp.float32)
    normed_two = norm_scale(middle_f, ffn_pre_gain).astype(jnp.bfloat16)
    full_linear, full_gated = (
        lax.all_gather(w_linear, "fs", axis=0, tiled=True),
        lax.all_gather(w_gated, "fs", axis=0, tiled=True),
    )
    linear = jnp.dot(normed_two, full_linear, preferred_element_type=jnp.float32)
    gated = jnp.dot(normed_two, full_gated, preferred_element_type=jnp.float32)
    linear = linear.astype(jnp.bfloat16)
    gated = gated.astype(jnp.bfloat16)
    activated = jax.nn.gelu(
        conv_three(gated.astype(jnp.float32), ffn_taps) + ffn_bias, approximate=True
    )
    hidden = (activated * linear.astype(jnp.float32)).astype(jnp.bfloat16)
    full_down = lax.all_gather(w_down, "fs", axis=1, tiled=True)
    partial_two = jnp.dot(hidden, full_down, preferred_element_type=jnp.float32)
    return settle(partial_two, middle_f, ffn_post_gain)


ORDER = (1, 3, 2)


def dot_nt(left, right):
    return lax.dot_general(left, right, (((1,), (1,)), ((), ())), preferred_element_type=jnp.float32)


def dot_nn(left, right):
    return jnp.dot(left, right, preferred_element_type=jnp.float32)


def conv_rows(values, taps):
    height = values.shape[0]
    row = lax.broadcasted_iota(jnp.int32, values.shape, 0) % SEQ_LEN
    before = jnp.where(row == 0, 0.0, pltpu.roll(values, 1, 0))
    after = jnp.where(row == SEQ_LEN - 1, 0.0, pltpu.roll(values, height - 1, 0))
    return taps[0:1] * before + taps[1:2] * values + taps[2:3] * after


def kernel(
    n_fs,
    conv_w,
    hid,
    stream,
    gains,
    mix_w,
    mix_taps,
    ffn_w,
    ffn_small,
    out,
    mix_all,
    ffn_all,
    xs,
    normed,
    middle,
    pm,
    rm,
    sm,
    rxm,
    bm,
    pf,
    rf,
    sf,
    rxf,
    tf,
    rz,
    bf,
    zs_s,
    zs_r,
    mix_s,
    mix_r,
    ag_s,
    ag_r,
    rs_s,
    rs_r,
    fin_s,
    fin_r,
):
    r, f, t = lax.axis_index("rep"), lax.axis_index("fs"), lax.axis_index("tp")
    x, c = t // 2, t % 2
    core = {"tp": 2 * x + 1 - c}
    side = {"tp": 2 * (1 - x) + c}
    t_side = 2 * (1 - x) + c
    other = {"rep": 1 - r}
    rows, width = stream.shape[0], mix_w.shape[1]
    n_seq = rows // SEQ_LEN
    mix_half, ffn_half = mix_w.shape[0] // 2, ffn_w.shape[1] // 2

    def send(src, dst, ss, rs, where):
        return pltpu.make_async_remote_copy(
            src_ref=src,
            dst_ref=dst,
            send_sem=ss,
            recv_sem=rs,
            device_id=where,
            device_id_type=pl.DeviceIdType.MESH,
        )

    barrier = pltpu.get_barrier_semaphore()
    peers = [core, side, other] + [{"fs": (f + k) % n_fs} for k in ORDER]
    for peer in peers:
        pl.semaphore_signal(barrier, inc=1, device_id=peer, device_id_type=pl.DeviceIdType.MESH)
    pl.semaphore_wait(barrier, len(peers))

    mix_rows = pl.ds(pl.multiple_of(r * mix_half, PACK), mix_half)
    ffn_rows = pl.ds(pl.multiple_of(r * ffn_half, PACK), ffn_half)
    mix_z, ffn_z = {}, {}
    for k in ORDER:
        to = {"fs": (f + k) % n_fs}
        mix_z[k] = send(mix_w.at[mix_rows], mix_all.at[f, mix_rows], zs_s.at[0, k], zs_r.at[0, k], to)
        mix_z[k].start()
    for k in ORDER:
        to = {"fs": (f + k) % n_fs}
        ffn_z[k] = send(
            ffn_w.at[(f + k) % n_fs, ffn_rows], ffn_all.at[f, ffn_rows], zs_s.at[1, k], zs_r.at[1, k], to
        )
        ffn_z[k].start()

    mix_all[f] = mix_w[...]
    ffn_all[f] = ffn_w[f]

    def norm_rows(values, gain):
        scale = lax.rsqrt(jnp.mean(values * values, axis=-1, keepdims=True) + EPS)
        return values * scale * gain

    step_rows = 32

    @pl.loop(0, rows // step_rows)
    def _(i):
        at = pl.ds(pl.multiple_of(i * step_rows, step_rows), step_rows)
        normed[at] = norm_rows(stream[at].astype(jnp.float32), gains[0:1]).astype(jnp.bfloat16)

    mix_y = {}
    for k in ORDER:
        mix_z[k].wait_recv()
        src = mix_all.at[(f - k + n_fs) % n_fs, mix_rows]
        mix_y[k] = send(src, src, zs_s.at[2, k], zs_r.at[2, k], other)
        mix_y[k].start()
    for k in ORDER:
        mix_y[k].wait_recv()

    mix_core, mix_side, mix_back = {}, {}, {}
    for q in range(n_seq):
        here = slice(q * SEQ_LEN, (q + 1) * SEQ_LEN)
        parts = []
        for p in range(3):
            total = 0.0
            for j in range(n_fs):
                total = total + dot_nt(
                    normed[here, j * width : (j + 1) * width], mix_all[j, p * conv_w : (p + 1) * conv_w]
                )
            parts.append(total.astype(jnp.bfloat16).astype(jnp.float32))
        mixed = (parts[0] * conv_rows(parts[1] * parts[2], mix_taps)).astype(jnp.bfloat16)
        for j in range(n_fs):
            pm[q, j % 2, j // 2] = dot_nn(mixed, mix_all[j, 3 * conv_w : 4 * conv_w]).astype(jnp.bfloat16)
        mix_core[q] = send(pm.at[q, 1 - c], rm.at[q], mix_s.at[0, q], mix_r.at[0, q], core)
        mix_core[q].start()
    for q in range(n_seq):
        mix_core[q].wait_recv()
        sm[q] = (pm[q, c].astype(jnp.float32) + rm[q].astype(jnp.float32)).astype(jnp.bfloat16)
        mix_side[q] = send(sm.at[q], rxm.at[q], mix_s.at[1, q], mix_r.at[1, q], side)
        mix_side[q].start()
    ffn_y = {}

    def forward(k):
        ffn_z[k].wait_recv()
        src = ffn_all.at[(f - k + n_fs) % n_fs, ffn_rows]
        ffn_y[k] = send(src, src, zs_s.at[3, k], zs_r.at[3, k], other)
        ffn_y[k].start()

    for q in range(n_seq):
        mix_side[q].wait_recv()
        bm[q, c] = (sm[q].astype(jnp.float32) + rxm[q].astype(jnp.float32)).astype(jnp.bfloat16)
        mix_back[q] = send(bm.at[q, c], bm.at[q, c], mix_s.at[2, q], mix_r.at[2, q], core)
        mix_back[q].start()
    for q in range(n_seq):
        mix_back[q].wait_recv()

        @pl.loop(0, SEQ_LEN // step_rows)
        def _(i):
            at = pl.ds(pl.multiple_of(i * step_rows, step_rows), step_rows)
            to = pl.ds(pl.multiple_of(q * SEQ_LEN + i * step_rows, step_rows), step_rows)
            branch = jnp.concatenate([bm[q, j % 2, j // 2, at] for j in range(n_fs)], axis=1)
            mid = stream[to].astype(jnp.float32) + norm_rows(branch.astype(jnp.float32), gains[1:2])
            mid = mid.astype(jnp.bfloat16)
            middle[to] = mid
            two = norm_rows(mid.astype(jnp.float32), gains[2:3]).astype(jnp.bfloat16)
            for j in range(n_fs):
                xs[f, j, to] = two[:, j * width : (j + 1) * width]

    ag_z, ag_side, ag_core, ag_fwd = {}, {}, {}, {}
    for k in ORDER:
        src = xs.at[f, t]
        ag_z[k] = send(src, src, ag_s.at[0, k], ag_r.at[0, k], {"fs": (f + k) % n_fs})
        ag_z[k].start()
    for k in ORDER:
        forward(k)

    def spread(k):
        ag_z[k].wait_recv()
        src = xs.at[(f - k + n_fs) % n_fs, t]
        ag_side[k] = send(src, src, ag_s.at[1, k], ag_r.at[1, k], side)
        ag_side[k].start()
        ag_core[k] = send(src, src, ag_s.at[2, k], ag_r.at[2, k], core)
        ag_core[k].start()

    def pass_on(k):
        ag_side[k].wait_recv()
        src = xs.at[(f - k + n_fs) % n_fs, t_side]
        ag_fwd[k] = send(src, src, ag_s.at[3, k], ag_r.at[3, k], core)
        ag_fwd[k].start()

    rs_core, rs_side, rs_z = {}, {}, {}

    def block(s):
        z = (f - s + n_fs) % n_fs
        small = ffn_small[f]

        @pl.loop(0, n_seq)
        def _(q):
            at = pl.ds(pl.multiple_of(q * SEQ_LEN, SEQ_LEN), SEQ_LEN)
            linear, gated = 0.0, 0.0
            for j in range(n_fs):
                act = xs[z, j, at]
                linear = linear + dot_nt(act, ffn_all[j, 0:hid])
                gated = gated + dot_nt(act, ffn_all[j, hid : 2 * hid])
            linear = linear.astype(jnp.bfloat16).astype(jnp.float32)
            gated = gated.astype(jnp.bfloat16).astype(jnp.float32)
            act = jax.nn.gelu(conv_rows(gated, small) + small[3:4], approximate=True)
            hidden = (act * linear).astype(jnp.bfloat16)
            for j in range(n_fs):
                pf[s, j % 2, j // 2, at] = dot_nn(hidden, ffn_all[j, 2 * hid : 3 * hid]).astype(jnp.bfloat16)

        rs_core[s] = send(pf.at[s, 1 - c], rf.at[s], rs_s.at[0, s], rs_r.at[0, s], core)
        rs_core[s].start()

    def stage_core(s):
        rs_core[s].wait_recv()
        sf[s, 1 - x] = (pf[s, c, 1 - x].astype(jnp.float32) + rf[s, 1 - x].astype(jnp.float32)).astype(jnp.bfloat16)
        rs_side[s] = send(sf.at[s, 1 - x], rxf.at[s], rs_s.at[1, s], rs_r.at[1, s], side)
        rs_side[s].start()
        sf[s, x] = (pf[s, c, x].astype(jnp.float32) + rf[s, x].astype(jnp.float32)).astype(jnp.bfloat16)

    def stage_side(s):
        rs_side[s].wait_recv()
        tf[s] = (sf[s, x].astype(jnp.float32) + rxf[s].astype(jnp.float32)).astype(jnp.bfloat16)
        if s > 0:
            rs_z[s] = send(tf.at[s], rz.at[s], rs_s.at[2, s], rs_r.at[2, s], {"fs": (f - s + n_fs) % n_fs})
            rs_z[s].start()

    for k in ORDER:
        ffn_y[k].wait_recv()
    block(0)
    spread(ORDER[0])
    stage_core(0)
    pass_on(ORDER[0])
    spread(ORDER[1])
    ag_core[ORDER[0]].wait_recv()
    ag_fwd[ORDER[0]].wait_recv()
    block(ORDER[0])
    pass_on(ORDER[1])
    spread(ORDER[2])
    stage_core(ORDER[0])
    ag_core[ORDER[1]].wait_recv()
    ag_fwd[ORDER[1]].wait_recv()
    block(ORDER[1])
    stage_side(0)
    pass_on(ORDER[2])
    stage_core(ORDER[1])
    stage_side(ORDER[0])
    ag_core[ORDER[2]].wait_recv()
    ag_fwd[ORDER[2]].wait_recv()
    block(ORDER[2])
    stage_core(ORDER[2])
    stage_side(ORDER[1])
    stage_side(ORDER[2])

    total = tf[0].astype(jnp.float32)
    for k in ORDER:
        rs_z[k].wait_recv()
        total = total + rz[k].astype(jnp.float32)
    bf[t] = total.astype(jnp.bfloat16)
    mine = bf.at[t]
    fin_side = send(mine, mine, fin_s.at[0], fin_r.at[0], side)
    fin_side.start()
    fin_core = send(mine, mine, fin_s.at[1], fin_r.at[1], core)
    fin_core.start()
    fin_side.wait_recv()
    theirs = bf.at[t_side]
    fin_fwd = send(theirs, theirs, fin_s.at[2], fin_r.at[2], core)
    fin_fwd.start()
    fin_core.wait_recv()
    fin_fwd.wait_recv()

    @pl.loop(0, rows // step_rows)
    def _(i):
        at = pl.ds(pl.multiple_of(i * step_rows, step_rows), step_rows)
        branch = jnp.concatenate([bf[j, at] for j in range(n_fs)], axis=1).astype(jnp.float32)
        out[at] = (middle[at].astype(jnp.float32) + norm_rows(branch, gains[3:4])).astype(jnp.bfloat16)

    groups = [mix_z, ffn_z, mix_y, ffn_y, mix_core, mix_side, mix_back]
    groups += [ag_z, ag_side, ag_core, ag_fwd, rs_core, rs_side, rs_z]
    for group in groups:
        for copy in group.values():
            copy.wait_send()
    for copy in (fin_side, fin_core, fin_fwd):
        copy.wait_send()


def split_plan(
    n_fs,
    stream,
    mix_pre_gain,
    w_outer_gate,
    w_inner_gate,
    w_value,
    mix_taps,
    w_mix_out,
    mix_post_gain,
    ffn_pre_gain,
    w_linear,
    w_gated,
    ffn_taps,
    ffn_bias,
    w_down,
    ffn_post_gain,
):
    rows, model = stream.shape
    width, conv_w = w_value.shape
    units = w_linear.shape[1] // n_fs
    hid = -(-units // PACK) * PACK
    deep = -(-3 * hid // (2 * PACK)) * 2 * PACK
    gains = jnp.stack([mix_pre_gain, mix_post_gain, ffn_pre_gain, ffn_post_gain])
    mix_w = jnp.concatenate([w_outer_gate.T, w_inner_gate.T, w_value.T, w_mix_out], axis=0)

    def cut(rows_of, extra):
        pieces = rows_of.reshape(n_fs, units, width)
        return jnp.pad(pieces, ((0, 0), (0, hid - units + extra), (0, 0)))

    ffn_w = jnp.concatenate([cut(w_linear.T, 0), cut(w_gated.T, 0), cut(w_down, deep - 3 * hid)], axis=1)
    small = jnp.concatenate([ffn_taps, ffn_bias[None]], axis=0).reshape(4, n_fs, units)
    small = jnp.pad(small.transpose(1, 0, 2), ((0, 0), (0, 0), (0, hid - units)))
    n_seq = rows // SEQ_LEN
    half = jnp.bfloat16
    vmem, dma = pltpu.VMEM, pltpu.SemaphoreType.DMA
    return pl.pallas_call(
        functools.partial(kernel, n_fs, conv_w, hid),
        out_shape=jax.ShapeDtypeStruct((rows, model), half),
        in_specs=[pl.BlockSpec(memory_space=vmem)] * 6,
        out_specs=pl.BlockSpec(memory_space=vmem),
        scratch_shapes=[
            vmem((n_fs, *mix_w.shape), half),
            vmem((n_fs, deep, width), half),
            vmem((n_fs, n_fs, rows, width), half),
            vmem((rows, model), half),
            vmem((rows, model), half),
            vmem((n_seq, 2, 2, SEQ_LEN, width), half),
            vmem((n_seq, 2, SEQ_LEN, width), half),
            vmem((n_seq, 2, SEQ_LEN, width), half),
            vmem((n_seq, 2, SEQ_LEN, width), half),
            vmem((n_seq, 2, 2, SEQ_LEN, width), half),
            vmem((n_fs, 2, 2, rows, width), half),
            vmem((n_fs, 2, rows, width), half),
            vmem((n_fs, 2, rows, width), half),
            vmem((n_fs, rows, width), half),
            vmem((n_fs, rows, width), half),
            vmem((n_fs, rows, width), half),
            vmem((n_fs, rows, width), half),
            dma((4, n_fs)),
            dma((4, n_fs)),
            dma((3, n_seq)),
            dma((3, n_seq)),
            dma((4, n_fs)),
            dma((4, n_fs)),
            dma((3, n_fs)),
            dma((3, n_fs)),
            dma((3,)),
            dma((3,)),
        ],
        compiler_params=pltpu.CompilerParams(
            collective_id=0, has_side_effects=True, vmem_limit_bytes=56 * 2**20
        ),
    )(stream, gains, mix_w, mix_taps, ffn_w, small)


def on_device(rep, n_fs, n_tp, *arrays):
    stream, w_value, w_linear = arrays[0], arrays[4], arrays[9]
    same = n_fs == n_tp == 2 * rep == len(ORDER) + 1
    whole = w_value.shape[0] % 128 == 0 and w_value.shape[1] % PACK == 0
    even = w_linear.shape[1] % n_fs == 0 and stream.shape[0] % SEQ_LEN == 0
    if same and rep == 2 and whole and even:
        return split_plan(n_fs, *arrays)
    return gather_plan(*arrays)


def solution(mesh):
    in_specs = (
        P(("rep", "fs"), None),
        P(),
        P("fs", "tp"),
        P("fs", "tp"),
        P("fs", "tp"),
        P(None, "tp"),
        P("tp", "fs"),
        P(),
        P(),
        P("fs", "tp"),
        P("fs", "tp"),
        P(None, "tp"),
        P("tp"),
        P("tp", "fs"),
        P(),
    )
    out_specs = P(("rep", "fs"), None)
    sizes = mesh.shape
    body = functools.partial(on_device, sizes["rep"], sizes["fs"], sizes["tp"])
    return jax.shard_map(
        body, mesh=mesh, in_specs=in_specs, out_specs=out_specs, check_vma=False
    )
```

```python
import functools

import jax
import jax.numpy as jnp
from jax import lax
from jax.experimental import pallas as pl
from jax.experimental.pallas import tpu as pltpu
from jax.sharding import PartitionSpec as P

SEQ_LEN = 128
PACK = 16


EPS = 1e-06


def norm_scale(values, gain):
    return values * lax.rsqrt(jnp.mean(values * values, axis=-1, keepdims=True) + EPS) * gain


def conv_three(values, taps):
    height, breadth = values.shape
    grouped = values.reshape(height // SEQ_LEN, SEQ_LEN, breadth)
    padded = jnp.pad(grouped, ((0, 0), (1, 1), (0, 0)))
    mixed = taps[0] * padded[:, :-2] + taps[1] * padded[:, 1:-1] + taps[2] * padded[:, 2:]
    return mixed.reshape(height, breadth)


def settle(partial_value, resid, post_gain):
    branch = lax.psum(partial_value.astype(jnp.bfloat16), "tp")
    return (resid + norm_scale(branch.astype(jnp.float32), post_gain)).astype(jnp.bfloat16)


def gather_plan(
    stream,
    mix_pre_gain,
    w_outer_gate,
    w_inner_gate,
    w_value,
    mix_taps,
    w_mix_out,
    mix_post_gain,
    ffn_pre_gain,
    w_linear,
    w_gated,
    ffn_taps,
    ffn_bias,
    w_down,
    ffn_post_gain,
):
    resid = stream.astype(jnp.float32)
    normed = norm_scale(resid, mix_pre_gain).astype(jnp.bfloat16)
    full_outer, full_inner, full_value = (
        lax.all_gather(w_outer_gate, "fs", axis=0, tiled=True),
        lax.all_gather(w_inner_gate, "fs", axis=0, tiled=True),
        lax.all_gather(w_value, "fs", axis=0, tiled=True),
    )
    outer = jnp.dot(normed, full_outer, preferred_element_type=jnp.float32)
    inner = jnp.dot(normed, full_inner, preferred_element_type=jnp.float32)
    value = jnp.dot(normed, full_value, preferred_element_type=jnp.float32)
    outer = outer.astype(jnp.bfloat16)
    inner = inner.astype(jnp.bfloat16)
    value = value.astype(jnp.bfloat16)
    product = inner.astype(jnp.float32) * value.astype(jnp.float32)
    mixed = (outer.astype(jnp.float32) * conv_three(product, mix_taps)).astype(jnp.bfloat16)
    full_mix_out = lax.all_gather(w_mix_out, "fs", axis=1, tiled=True)
    partial_value = jnp.dot(mixed, full_mix_out, preferred_element_type=jnp.float32)
    middle = settle(partial_value, resid, mix_post_gain)
    middle_f = middle.astype(jnp.float32)
    normed_two = norm_scale(middle_f, ffn_pre_gain).astype(jnp.bfloat16)
    full_linear, full_gated = (
        lax.all_gather(w_linear, "fs", axis=0, tiled=True),
        lax.all_gather(w_gated, "fs", axis=0, tiled=True),
    )
    linear = jnp.dot(normed_two, full_linear, preferred_element_type=jnp.float32)
    gated = jnp.dot(normed_two, full_gated, preferred_element_type=jnp.float32)
    linear = linear.astype(jnp.bfloat16)
    gated = gated.astype(jnp.bfloat16)
    activated = jax.nn.gelu(
        conv_three(gated.astype(jnp.float32), ffn_taps) + ffn_bias, approximate=True
    )
    hidden = (activated * linear.astype(jnp.float32)).astype(jnp.bfloat16)
    full_down = lax.all_gather(w_down, "fs", axis=1, tiled=True)
    partial_two = jnp.dot(hidden, full_down, preferred_element_type=jnp.float32)
    return settle(partial_two, middle_f, ffn_post_gain)


ORDER = (1, 3, 2)


def dot_nt(left, right):
    return lax.dot_general(left, right, (((1,), (1,)), ((), ())), preferred_element_type=jnp.float32)


def dot_nn(left, right):
    return jnp.dot(left, right, preferred_element_type=jnp.float32)


def conv_rows(values, taps):
    height = values.shape[0]
    row = lax.broadcasted_iota(jnp.int32, values.shape, 0) % SEQ_LEN
    before = jnp.where(row == 0, 0.0, pltpu.roll(values, 1, 0))
    after = jnp.where(row == SEQ_LEN - 1, 0.0, pltpu.roll(values, height - 1, 0))
    return taps[0:1] * before + taps[1:2] * values + taps[2:3] * after


def kernel(
    n_fs,
    conv_w,
    hid,
    stream,
    gain_mix_pre,
    gain_mix_post,
    gain_ffn_pre,
    gain_ffn_post,
    w_outer,
    w_inner,
    w_value,
    w_mix_out,
    mix_taps,
    w_linear,
    w_gated,
    w_down,
    ffn_taps,
    ffn_bias,
    out,
    small_all,
    ffn_w,
    mix_all,
    ffn_all,
    xs,
    normed,
    middle,
    pm,
    rm,
    sm,
    rxm,
    bm,
    pf,
    rf,
    sf,
    rxf,
    tf,
    rz,
    bf,
    zs_s,
    zs_r,
    mix_s,
    mix_r,
    ag_s,
    ag_r,
    rs_s,
    rs_r,
    fin_s,
    fin_r,
):
    r, f, t = lax.axis_index("rep"), lax.axis_index("fs"), lax.axis_index("tp")
    x, c = t // 2, t % 2
    core = {"tp": 2 * x + 1 - c}
    side = {"tp": 2 * (1 - x) + c}
    t_side = 2 * (1 - x) + c
    other = {"rep": 1 - r}
    rows, width = stream.shape[0], w_value.shape[1]
    units = w_linear.shape[1]
    n_seq = rows // SEQ_LEN
    mix_half, ffn_half = mix_all.shape[1] // 2, ffn_w.shape[1] // 2

    def send(src, dst, ss, rs, where):
        return pltpu.make_async_remote_copy(
            src_ref=src,
            dst_ref=dst,
            send_sem=ss,
            recv_sem=rs,
            device_id=where,
            device_id_type=pl.DeviceIdType.MESH,
        )

    barrier = pltpu.get_barrier_semaphore()
    peers = [core, side, other] + [{"fs": (f + k) % n_fs} for k in ORDER]
    for peer in peers:
        pl.semaphore_signal(barrier, inc=1, device_id=peer, device_id_type=pl.DeviceIdType.MESH)
    for p, piece in enumerate((w_outer, w_inner, w_value, w_mix_out)):
        mix_all[f, p * conv_w : (p + 1) * conv_w] = piece[...]
    pl.semaphore_wait(barrier, len(peers))

    mix_rows = pl.ds(pl.multiple_of(r * mix_half, PACK), mix_half)
    ffn_rows = pl.ds(pl.multiple_of(r * ffn_half, PACK), ffn_half)
    mix_z, ffn_z = {}, {}
    for k in ORDER:
        to = {"fs": (f + k) % n_fs}
        mix_z[k] = send(mix_all.at[f, mix_rows], mix_all.at[f, mix_rows], zs_s.at[0, k], zs_r.at[0, k], to)
        mix_z[k].start()
    for p, piece in enumerate((w_linear, w_gated, w_down)):
        end = (p + 1) * hid if p < 2 else ffn_w.shape[1]
        edge = units // PACK * PACK
        for j in range(n_fs):
            ffn_w[j, p * hid + edge : end] = jnp.zeros((end - p * hid - edge, width), ffn_w.dtype)
            ffn_w[j, p * hid : p * hid + units] = piece[j]
    for k in ORDER:
        to = {"fs": (f + k) % n_fs}
        ffn_z[k] = send(
            ffn_w.at[(f + k) % n_fs, ffn_rows], ffn_all.at[f, ffn_rows], zs_s.at[1, k], zs_r.at[1, k], to
        )
        ffn_z[k].start()

    ffn_all[f] = ffn_w[f]
    small_all[...] = jnp.zeros(small_all.shape, jnp.float32)
    for j in range(n_fs):
        small_all[j, 0:3, 0:units] = ffn_taps[:, j * units : (j + 1) * units]
        small_all[j, 3:4, 0:units] = ffn_bias[j * units : (j + 1) * units][None]

    def norm_rows(values, gain):
        scale = lax.rsqrt(jnp.mean(values * values, axis=-1, keepdims=True) + EPS)
        return values * scale * gain

    step_rows = 32

    @pl.loop(0, rows // step_rows)
    def _(i):
        at = pl.ds(pl.multiple_of(i * step_rows, step_rows), step_rows)
        normed[at] = norm_rows(stream[at].astype(jnp.float32), gain_mix_pre[...][None]).astype(jnp.bfloat16)

    mix_y = {}
    for k in ORDER:
        mix_z[k].wait_recv()
        src = mix_all.at[(f - k + n_fs) % n_fs, mix_rows]
        mix_y[k] = send(src, src, zs_s.at[2, k], zs_r.at[2, k], other)
        mix_y[k].start()
    for k in ORDER:
        mix_y[k].wait_recv()

    mix_core, mix_side, mix_back = {}, {}, {}
    for q in range(n_seq):
        here = slice(q * SEQ_LEN, (q + 1) * SEQ_LEN)
        parts = []
        for p in range(3):
            total = 0.0
            for j in range(n_fs):
                total = total + dot_nt(
                    normed[here, j * width : (j + 1) * width], mix_all[j, p * conv_w : (p + 1) * conv_w]
                )
            parts.append(total.astype(jnp.bfloat16).astype(jnp.float32))
        mixed = (parts[0] * conv_rows(parts[1] * parts[2], mix_taps)).astype(jnp.bfloat16)
        for j in range(n_fs):
            pm[q, j % 2, j // 2] = dot_nn(mixed, mix_all[j, 3 * conv_w : 4 * conv_w]).astype(jnp.bfloat16)
        mix_core[q] = send(pm.at[q, 1 - c], rm.at[q], mix_s.at[0, q], mix_r.at[0, q], core)
        mix_core[q].start()
    for q in range(n_seq):
        mix_core[q].wait_recv()
        sm[q] = (pm[q, c].astype(jnp.float32) + rm[q].astype(jnp.float32)).astype(jnp.bfloat16)
        mix_side[q] = send(sm.at[q], rxm.at[q], mix_s.at[1, q], mix_r.at[1, q], side)
        mix_side[q].start()
    ffn_y = {}

    def forward(k):
        ffn_z[k].wait_recv()
        src = ffn_all.at[(f - k + n_fs) % n_fs, ffn_rows]
        ffn_y[k] = send(src, src, zs_s.at[3, k], zs_r.at[3, k], other)
        ffn_y[k].start()

    for q in range(n_seq):
        mix_side[q].wait_recv()
        bm[q, c] = (sm[q].astype(jnp.float32) + rxm[q].astype(jnp.float32)).astype(jnp.bfloat16)
        mix_back[q] = send(bm.at[q, c], bm.at[q, c], mix_s.at[2, q], mix_r.at[2, q], core)
        mix_back[q].start()
    ag_z, ag_side, ag_core, ag_fwd = {}, {}, {}, {}
    forward(ORDER[0])
    forward(ORDER[1])
    for q in range(n_seq):
        mix_back[q].wait_recv()

        @pl.loop(0, SEQ_LEN // step_rows)
        def _(i):
            at = pl.ds(pl.multiple_of(i * step_rows, step_rows), step_rows)
            to = pl.ds(pl.multiple_of(q * SEQ_LEN + i * step_rows, step_rows), step_rows)
            branch = jnp.concatenate([bm[q, j % 2, j // 2, at] for j in range(n_fs)], axis=1)
            mid = stream[to].astype(jnp.float32) + norm_rows(branch.astype(jnp.float32), gain_mix_post[...][None])
            mid = mid.astype(jnp.bfloat16)
            middle[to] = mid
            two = norm_rows(mid.astype(jnp.float32), gain_ffn_pre[...][None]).astype(jnp.bfloat16)
            for j in range(n_fs):
                xs[f, j, to] = two[:, j * width : (j + 1) * width]

        for k in ORDER:
            src = xs.at[f, t, q * SEQ_LEN : (q + 1) * SEQ_LEN]
            ag_z[k, q] = send(src, src, ag_s.at[0, k, q], ag_r.at[0, k, q], {"fs": (f + k) % n_fs})
            ag_z[k, q].start()

    forward(ORDER[2])

    def spread(k, q):
        ag_z[k, q].wait_recv()
        src = xs.at[(f - k + n_fs) % n_fs, t, q * SEQ_LEN : (q + 1) * SEQ_LEN]
        ag_side[k, q] = send(src, src, ag_s.at[1, k, q], ag_r.at[1, k, q], side)
        ag_side[k, q].start()
        ag_core[k, q] = send(src, src, ag_s.at[2, k, q], ag_r.at[2, k, q], core)
        ag_core[k, q].start()

    def pass_on(k, q):
        ag_side[k, q].wait_recv()
        src = xs.at[(f - k + n_fs) % n_fs, t_side, q * SEQ_LEN : (q + 1) * SEQ_LEN]
        ag_fwd[k, q] = send(src, src, ag_s.at[3, k, q], ag_r.at[3, k, q], core)
        ag_fwd[k, q].start()

    rs_core, rs_side, rs_z = {}, {}, {}

    def block(k, q):
        if k > 0:
            ag_core[k, q].wait_recv()
            ag_fwd[k, q].wait_recv()
        z = (f - k + n_fs) % n_fs
        small = small_all[f]
        linear, gated = 0.0, 0.0
        for j in range(n_fs):
            act = xs[z, j, q * SEQ_LEN : (q + 1) * SEQ_LEN]
            linear = linear + dot_nt(act, ffn_all[j, 0:hid])
            gated = gated + dot_nt(act, ffn_all[j, hid : 2 * hid])
        linear = linear.astype(jnp.bfloat16).astype(jnp.float32)
        gated = gated.astype(jnp.bfloat16).astype(jnp.float32)
        act = jax.nn.gelu(conv_rows(gated, small) + small[3:4], approximate=True)
        hidden = (act * linear).astype(jnp.bfloat16)
        for j in range(n_fs):
            pf[k, q, j % 2, j // 2] = dot_nn(hidden, ffn_all[j, 2 * hid : 3 * hid]).astype(jnp.bfloat16)
        rs_core[k, q] = send(pf.at[k, q, 1 - c], rf.at[k, q], rs_s.at[0, k, q], rs_r.at[0, k, q], core)
        rs_core[k, q].start()

    def stage_core(k, q):
        rs_core[k, q].wait_recv()
        theirs = pf[k, q, c, 1 - x].astype(jnp.float32) + rf[k, q, 1 - x].astype(jnp.float32)
        sf[k, q, 1 - x] = theirs.astype(jnp.bfloat16)
        rs_side[k, q] = send(sf.at[k, q, 1 - x], rxf.at[k, q], rs_s.at[1, k, q], rs_r.at[1, k, q], side)
        rs_side[k, q].start()
        ours = pf[k, q, c, x].astype(jnp.float32) + rf[k, q, x].astype(jnp.float32)
        sf[k, q, x] = ours.astype(jnp.bfloat16)

    def stage_side(k, q):
        rs_side[k, q].wait_recv()
        tf[k, q] = (sf[k, q, x].astype(jnp.float32) + rxf[k, q].astype(jnp.float32)).astype(jnp.bfloat16)
        if k > 0:
            to = {"fs": (f - k + n_fs) % n_fs}
            rs_z[k, q] = send(tf.at[k, q], rz.at[k, q], rs_s.at[2, k, q], rs_r.at[2, k, q], to)
            rs_z[k, q].start()

    for k in ORDER:
        ffn_y[k].wait_recv()
    own = [(0, q) for q in range(n_seq)]
    work = [(k, q) for k in ORDER for q in range(n_seq)]
    lag = len(own)
    every = own + work
    for i in range(len(work) + 6):
        if i < len(work):
            spread(*work[i])
        if i < lag:
            block(*own[i])
        if 1 <= i <= len(work):
            pass_on(*work[i - 1])
        if 2 <= i < len(work) + 2:
            block(*work[i - 2])
        if 1 <= i <= len(every):
            stage_core(*every[i - 1])
        if 3 <= i < len(every) + 3:
            stage_side(*every[i - 3])

    fin_side, fin_core, fin_fwd = {}, {}, {}
    for q in range(n_seq):
        at = slice(q * SEQ_LEN, (q + 1) * SEQ_LEN)
        total = tf[0, q].astype(jnp.float32)
        for k in ORDER:
            rs_z[k, q].wait_recv()
            total = total + rz[k, q].astype(jnp.float32)
        bf[t, at] = total.astype(jnp.bfloat16)
        mine = bf.at[t, at]
        fin_side[q] = send(mine, mine, fin_s.at[0, q], fin_r.at[0, q], side)
        fin_side[q].start()
        fin_core[q] = send(mine, mine, fin_s.at[1, q], fin_r.at[1, q], core)
        fin_core[q].start()
    for q in range(n_seq):
        fin_side[q].wait_recv()
        theirs = bf.at[t_side, q * SEQ_LEN : (q + 1) * SEQ_LEN]
        fin_fwd[q] = send(theirs, theirs, fin_s.at[2, q], fin_r.at[2, q], core)
        fin_fwd[q].start()
    for q in range(n_seq):
        fin_core[q].wait_recv()
        fin_fwd[q].wait_recv()

    @pl.loop(0, rows // step_rows)
    def _(i):
        at = pl.ds(pl.multiple_of(i * step_rows, step_rows), step_rows)
        branch = jnp.concatenate([bf[j, at] for j in range(n_fs)], axis=1).astype(jnp.float32)
        out[at] = (middle[at].astype(jnp.float32) + norm_rows(branch, gain_ffn_post[...][None])).astype(jnp.bfloat16)

    groups = [mix_z, ffn_z, mix_y, ffn_y, mix_core, mix_side, mix_back]
    groups += [ag_z, ag_side, ag_core, ag_fwd, rs_core, rs_side, rs_z]
    groups += [fin_side, fin_core, fin_fwd]
    for group in groups:
        for copy in group.values():
            copy.wait_send()


def split_plan(
    n_fs,
    stream,
    mix_pre_gain,
    w_outer_gate,
    w_inner_gate,
    w_value,
    mix_taps,
    w_mix_out,
    mix_post_gain,
    ffn_pre_gain,
    w_linear,
    w_gated,
    ffn_taps,
    ffn_bias,
    w_down,
    ffn_post_gain,
):
    rows, model = stream.shape
    width, conv_w = w_value.shape
    units = w_linear.shape[1] // n_fs
    hid = -(-units // PACK) * PACK
    deep = -(-3 * hid // (2 * PACK)) * 2 * PACK
    cut = lambda rows_of: rows_of.reshape(n_fs, units, width)
    n_seq = rows // SEQ_LEN
    half = jnp.bfloat16
    vmem, dma = pltpu.VMEM, pltpu.SemaphoreType.DMA
    return pl.pallas_call(
        functools.partial(kernel, n_fs, conv_w, hid),
        out_shape=jax.ShapeDtypeStruct((rows, model), half),
        in_specs=[pl.BlockSpec(memory_space=vmem)] * 15,
        out_specs=pl.BlockSpec(memory_space=vmem),
        scratch_shapes=[
            vmem((n_fs, 8, hid), jnp.float32),
            vmem((n_fs, deep, width), half),
            vmem((n_fs, 4 * conv_w, width), half),
            vmem((n_fs, deep, width), half),
            vmem((n_fs, n_fs, rows, width), half),
            vmem((rows, model), half),
            vmem((rows, model), half),
            vmem((n_seq, 2, 2, SEQ_LEN, width), half),
            vmem((n_seq, 2, SEQ_LEN, width), half),
            vmem((n_seq, 2, SEQ_LEN, width), half),
            vmem((n_seq, 2, SEQ_LEN, width), half),
            vmem((n_seq, 2, 2, SEQ_LEN, width), half),
            vmem((n_fs, n_seq, 2, 2, SEQ_LEN, width), half),
            vmem((n_fs, n_seq, 2, SEQ_LEN, width), half),
            vmem((n_fs, n_seq, 2, SEQ_LEN, width), half),
            vmem((n_fs, n_seq, SEQ_LEN, width), half),
            vmem((n_fs, n_seq, SEQ_LEN, width), half),
            vmem((n_fs, n_seq, SEQ_LEN, width), half),
            vmem((n_fs, rows, width), half),
            dma((4, n_fs)),
            dma((4, n_fs)),
            dma((3, n_seq)),
            dma((3, n_seq)),
            dma((4, n_fs, n_seq)),
            dma((4, n_fs, n_seq)),
            dma((3, n_fs, n_seq)),
            dma((3, n_fs, n_seq)),
            dma((3, n_seq)),
            dma((3, n_seq)),
        ],
        compiler_params=pltpu.CompilerParams(
            collective_id=0, has_side_effects=True, vmem_limit_bytes=56 * 2**20
        ),
    )(
        stream,
        mix_pre_gain,
        mix_post_gain,
        ffn_pre_gain,
        ffn_post_gain,
        w_outer_gate.T,
        w_inner_gate.T,
        w_value.T,
        w_mix_out,
        mix_taps,
        cut(w_linear.T),
        cut(w_gated.T),
        cut(w_down),
        ffn_taps,
        ffn_bias,
    )


def on_device(rep, n_fs, n_tp, *arrays):
    stream, w_value, w_linear = arrays[0], arrays[4], arrays[9]
    same = n_fs == n_tp == 2 * rep == len(ORDER) + 1
    whole = w_value.shape[0] % 128 == 0 and w_value.shape[1] % PACK == 0
    even = w_linear.shape[1] % n_fs == 0 and stream.shape[0] % SEQ_LEN == 0
    if same and rep == 2 and whole and even:
        return split_plan(n_fs, *arrays)
    return gather_plan(*arrays)


def solution(mesh):
    in_specs = (
        P(("rep", "fs"), None),
        P(),
        P("fs", "tp"),
        P("fs", "tp"),
        P("fs", "tp"),
        P(None, "tp"),
        P("tp", "fs"),
        P(),
        P(),
        P("fs", "tp"),
        P("fs", "tp"),
        P(None, "tp"),
        P("tp"),
        P("tp", "fs"),
        P(),
    )
    out_specs = P(("rep", "fs"), None)
    sizes = mesh.shape
    body = functools.partial(on_device, sizes["rep"], sizes["fs"], sizes["tp"])
    return jax.shard_map(
        body, mesh=mesh, in_specs=in_specs, out_specs=out_specs, check_vma=False
    )
```

```python
import functools

import jax
import jax.numpy as jnp
from jax import lax
from jax.experimental import pallas as pl
from jax.experimental.pallas import tpu as pltpu
from jax.sharding import PartitionSpec as P

SEQ_LEN = 128
PACK = 16
CHUNKS = 2


EPS = 1e-06


def norm_scale(values, gain):
    return values * lax.rsqrt(jnp.mean(values * values, axis=-1, keepdims=True) + EPS) * gain


def conv_three(values, taps):
    height, breadth = values.shape
    grouped = values.reshape(height // SEQ_LEN, SEQ_LEN, breadth)
    padded = jnp.pad(grouped, ((0, 0), (1, 1), (0, 0)))
    mixed = taps[0] * padded[:, :-2] + taps[1] * padded[:, 1:-1] + taps[2] * padded[:, 2:]
    return mixed.reshape(height, breadth)


def settle(partial_value, resid, post_gain):
    branch = lax.psum(partial_value.astype(jnp.bfloat16), "tp")
    return (resid + norm_scale(branch.astype(jnp.float32), post_gain)).astype(jnp.bfloat16)


def gather_plan(
    stream,
    mix_pre_gain,
    w_outer_gate,
    w_inner_gate,
    w_value,
    mix_taps,
    w_mix_out,
    mix_post_gain,
    ffn_pre_gain,
    w_linear,
    w_gated,
    ffn_taps,
    ffn_bias,
    w_down,
    ffn_post_gain,
):
    resid = stream.astype(jnp.float32)
    normed = norm_scale(resid, mix_pre_gain).astype(jnp.bfloat16)
    full_outer, full_inner, full_value = (
        lax.all_gather(w_outer_gate, "fs", axis=0, tiled=True),
        lax.all_gather(w_inner_gate, "fs", axis=0, tiled=True),
        lax.all_gather(w_value, "fs", axis=0, tiled=True),
    )
    outer = jnp.dot(normed, full_outer, preferred_element_type=jnp.float32)
    inner = jnp.dot(normed, full_inner, preferred_element_type=jnp.float32)
    value = jnp.dot(normed, full_value, preferred_element_type=jnp.float32)
    outer = outer.astype(jnp.bfloat16)
    inner = inner.astype(jnp.bfloat16)
    value = value.astype(jnp.bfloat16)
    product = inner.astype(jnp.float32) * value.astype(jnp.float32)
    mixed = (outer.astype(jnp.float32) * conv_three(product, mix_taps)).astype(jnp.bfloat16)
    full_mix_out = lax.all_gather(w_mix_out, "fs", axis=1, tiled=True)
    partial_value = jnp.dot(mixed, full_mix_out, preferred_element_type=jnp.float32)
    middle = settle(partial_value, resid, mix_post_gain)
    middle_f = middle.astype(jnp.float32)
    normed_two = norm_scale(middle_f, ffn_pre_gain).astype(jnp.bfloat16)
    full_linear, full_gated = (
        lax.all_gather(w_linear, "fs", axis=0, tiled=True),
        lax.all_gather(w_gated, "fs", axis=0, tiled=True),
    )
    linear = jnp.dot(normed_two, full_linear, preferred_element_type=jnp.float32)
    gated = jnp.dot(normed_two, full_gated, preferred_element_type=jnp.float32)
    linear = linear.astype(jnp.bfloat16)
    gated = gated.astype(jnp.bfloat16)
    activated = jax.nn.gelu(
        conv_three(gated.astype(jnp.float32), ffn_taps) + ffn_bias, approximate=True
    )
    hidden = (activated * linear.astype(jnp.float32)).astype(jnp.bfloat16)
    full_down = lax.all_gather(w_down, "fs", axis=1, tiled=True)
    partial_two = jnp.dot(hidden, full_down, preferred_element_type=jnp.float32)
    return settle(partial_two, middle_f, ffn_post_gain)


ORDER = (1, 3, 2)


def dot_nt(left, right):
    return lax.dot_general(left, right, (((1,), (1,)), ((), ())), preferred_element_type=jnp.float32)


def dot_nn(left, right):
    return jnp.dot(left, right, preferred_element_type=jnp.float32)


def conv_rows(values, taps):
    height = values.shape[0]
    row = lax.broadcasted_iota(jnp.int32, values.shape, 0) % SEQ_LEN
    before = jnp.where(row == 0, 0.0, pltpu.roll(values, 1, 0))
    after = jnp.where(row == SEQ_LEN - 1, 0.0, pltpu.roll(values, height - 1, 0))
    return taps[0:1] * before + taps[1:2] * values + taps[2:3] * after


def kernel(
    n_fs,
    conv_w,
    hid,
    stream,
    gain_mix_pre,
    gain_mix_post,
    gain_ffn_pre,
    gain_ffn_post,
    w_outer,
    w_inner,
    w_value,
    w_mix_out,
    mix_taps,
    w_linear,
    w_gated,
    w_down,
    ffn_taps,
    ffn_bias,
    out,
    small_all,
    ffn_w,
    mix_all,
    ffn_all,
    xs,
    normed,
    middle,
    pm,
    rm,
    sm,
    rxm,
    bm,
    pf,
    rf,
    sf,
    rxf,
    tf,
    rz,
    bf,
    zs_s,
    zs_r,
    mix_s,
    mix_r,
    ag_s,
    ag_r,
    rs_s,
    rs_r,
    fin_s,
    fin_r,
):
    r, f, t = lax.axis_index("rep"), lax.axis_index("fs"), lax.axis_index("tp")
    x, c = t // 2, t % 2
    core = {"tp": 2 * x + 1 - c}
    side = {"tp": 2 * (1 - x) + c}
    t_side = 2 * (1 - x) + c
    other = {"rep": 1 - r}
    rows, width = stream.shape[0], w_value.shape[1]
    units = w_linear.shape[1]
    n_seq = rows // SEQ_LEN
    mix_half, ffn_half = mix_all.shape[1] // 2, ffn_w.shape[1] // 2

    def send(src, dst, ss, rs, where):
        return pltpu.make_async_remote_copy(
            src_ref=src,
            dst_ref=dst,
            send_sem=ss,
            recv_sem=rs,
            device_id=where,
            device_id_type=pl.DeviceIdType.MESH,
        )

    barrier = pltpu.get_barrier_semaphore()
    peers = [core, side, other] + [{"fs": (f + k) % n_fs} for k in ORDER]
    for peer in peers:
        pl.semaphore_signal(barrier, inc=1, device_id=peer, device_id_type=pl.DeviceIdType.MESH)
    for p, piece in enumerate((w_outer, w_inner, w_value, w_mix_out)):
        mix_all[f, p * conv_w : (p + 1) * conv_w] = piece[...]
    pl.semaphore_wait(barrier, len(peers))

    mix_cut, ffn_cut = mix_half // CHUNKS, ffn_half // CHUNKS
    mix_rows = [pl.ds(pl.multiple_of(r * mix_half + h * mix_cut, PACK), mix_cut) for h in range(CHUNKS)]
    ffn_rows = [pl.ds(pl.multiple_of(r * ffn_half + h * ffn_cut, PACK), ffn_cut) for h in range(CHUNKS)]
    cuts = [(k, h) for k in ORDER for h in range(CHUNKS)]
    mix_z, ffn_z = {}, {}
    for k, h in cuts:
        to = {"fs": (f + k) % n_fs}
        src = mix_all.at[f, mix_rows[h]]
        mix_z[k, h] = send(src, src, zs_s.at[0, k, h], zs_r.at[0, k, h], to)
        mix_z[k, h].start()
    for p, piece in enumerate((w_linear, w_gated, w_down)):
        end = (p + 1) * hid if p < 2 else ffn_w.shape[1]
        edge = units // PACK * PACK
        for j in range(n_fs):
            ffn_w[j, p * hid + edge : end] = jnp.zeros((end - p * hid - edge, width), ffn_w.dtype)
            ffn_w[j, p * hid : p * hid + units] = piece[j]
    for k, h in cuts:
        to = (f + k) % n_fs
        src, dst = ffn_w.at[to, ffn_rows[h]], ffn_all.at[f, ffn_rows[h]]
        ffn_z[k, h] = send(src, dst, zs_s.at[1, k, h], zs_r.at[1, k, h], {"fs": to})
        ffn_z[k, h].start()

    ffn_all[f] = ffn_w[f]
    small_all[...] = jnp.zeros(small_all.shape, jnp.float32)
    for j in range(n_fs):
        small_all[j, 0:3, 0:units] = ffn_taps[:, j * units : (j + 1) * units]
        small_all[j, 3:4, 0:units] = ffn_bias[j * units : (j + 1) * units][None]

    def norm_rows(values, gain):
        scale = lax.rsqrt(jnp.mean(values * values, axis=-1, keepdims=True) + EPS)
        return values * scale * gain

    step_rows = 32

    @pl.loop(0, rows // step_rows)
    def _(i):
        at = pl.ds(pl.multiple_of(i * step_rows, step_rows), step_rows)
        normed[at] = norm_rows(stream[at].astype(jnp.float32), gain_mix_pre[...][None]).astype(jnp.bfloat16)

    mix_y = {}
    for k, h in cuts:
        mix_z[k, h].wait_recv()
        src = mix_all.at[(f - k + n_fs) % n_fs, mix_rows[h]]
        mix_y[k, h] = send(src, src, zs_s.at[2, k, h], zs_r.at[2, k, h], other)
        mix_y[k, h].start()
    for k, h in cuts:
        mix_y[k, h].wait_recv()

    mix_core, mix_side, mix_back = {}, {}, {}
    for q in range(n_seq):
        here = slice(q * SEQ_LEN, (q + 1) * SEQ_LEN)
        parts = []
        for p in range(3):
            total = 0.0
            for j in range(n_fs):
                total = total + dot_nt(
                    normed[here, j * width : (j + 1) * width], mix_all[j, p * conv_w : (p + 1) * conv_w]
                )
            parts.append(total.astype(jnp.bfloat16).astype(jnp.float32))
        mixed = (parts[0] * conv_rows(parts[1] * parts[2], mix_taps)).astype(jnp.bfloat16)
        for j in range(n_fs):
            pm[q, j % 2, j // 2] = dot_nn(mixed, mix_all[j, 3 * conv_w : 4 * conv_w]).astype(jnp.bfloat16)
        mix_core[q] = send(pm.at[q, 1 - c], rm.at[q], mix_s.at[0, q], mix_r.at[0, q], core)
        mix_core[q].start()
    for q in range(n_seq):
        mix_core[q].wait_recv()
        sm[q] = (pm[q, c].astype(jnp.float32) + rm[q].astype(jnp.float32)).astype(jnp.bfloat16)
        mix_side[q] = send(sm.at[q], rxm.at[q], mix_s.at[1, q], mix_r.at[1, q], side)
        mix_side[q].start()
    ffn_y = {}

    def forward(k):
        for h in range(CHUNKS):
            ffn_z[k, h].wait_recv()
            src = ffn_all.at[(f - k + n_fs) % n_fs, ffn_rows[h]]
            ffn_y[k, h] = send(src, src, zs_s.at[3, k, h], zs_r.at[3, k, h], other)
            ffn_y[k, h].start()

    for q in range(n_seq):
        mix_side[q].wait_recv()
        bm[q, c] = (sm[q].astype(jnp.float32) + rxm[q].astype(jnp.float32)).astype(jnp.bfloat16)
        mix_back[q] = send(bm.at[q, c], bm.at[q, c], mix_s.at[2, q], mix_r.at[2, q], core)
        mix_back[q].start()
    ag_z, ag_side, ag_core, ag_fwd = {}, {}, {}, {}
    forward(ORDER[0])
    forward(ORDER[1])
    for q in range(n_seq):
        mix_back[q].wait_recv()

        @pl.loop(0, SEQ_LEN // step_rows)
        def _(i):
            at = pl.ds(pl.multiple_of(i * step_rows, step_rows), step_rows)
            to = pl.ds(pl.multiple_of(q * SEQ_LEN + i * step_rows, step_rows), step_rows)
            branch = jnp.concatenate([bm[q, j % 2, j // 2, at] for j in range(n_fs)], axis=1)
            mid = stream[to].astype(jnp.float32) + norm_rows(branch.astype(jnp.float32), gain_mix_post[...][None])
            mid = mid.astype(jnp.bfloat16)
            middle[to] = mid
            two = norm_rows(mid.astype(jnp.float32), gain_ffn_pre[...][None]).astype(jnp.bfloat16)
            for j in range(n_fs):
                xs[f, j, to] = two[:, j * width : (j + 1) * width]

        for k in ORDER:
            src = xs.at[f, t, q * SEQ_LEN : (q + 1) * SEQ_LEN]
            ag_z[k, q] = send(src, src, ag_s.at[0, k, q], ag_r.at[0, k, q], {"fs": (f + k) % n_fs})
            ag_z[k, q].start()

    forward(ORDER[2])

    def spread(k, q):
        ag_z[k, q].wait_recv()
        src = xs.at[(f - k + n_fs) % n_fs, t, q * SEQ_LEN : (q + 1) * SEQ_LEN]
        ag_side[k, q] = send(src, src, ag_s.at[1, k, q], ag_r.at[1, k, q], side)
        ag_side[k, q].start()
        ag_core[k, q] = send(src, src, ag_s.at[2, k, q], ag_r.at[2, k, q], core)
        ag_core[k, q].start()

    def pass_on(k, q):
        ag_side[k, q].wait_recv()
        src = xs.at[(f - k + n_fs) % n_fs, t_side, q * SEQ_LEN : (q + 1) * SEQ_LEN]
        ag_fwd[k, q] = send(src, src, ag_s.at[3, k, q], ag_r.at[3, k, q], core)
        ag_fwd[k, q].start()

    rs_core, rs_side, rs_z = {}, {}, {}

    def block(k, q):
        if k > 0:
            ag_core[k, q].wait_recv()
            ag_fwd[k, q].wait_recv()
        z = (f - k + n_fs) % n_fs
        small = small_all[f]
        linear, gated = 0.0, 0.0
        for j in range(n_fs):
            act = xs[z, j, q * SEQ_LEN : (q + 1) * SEQ_LEN]
            linear = linear + dot_nt(act, ffn_all[j, 0:hid])
            gated = gated + dot_nt(act, ffn_all[j, hid : 2 * hid])
        linear = linear.astype(jnp.bfloat16).astype(jnp.float32)
        gated = gated.astype(jnp.bfloat16).astype(jnp.float32)
        act = jax.nn.gelu(conv_rows(gated, small) + small[3:4], approximate=True)
        hidden = (act * linear).astype(jnp.bfloat16)
        for j in range(n_fs):
            pf[k, q, j % 2, j // 2] = dot_nn(hidden, ffn_all[j, 2 * hid : 3 * hid]).astype(jnp.bfloat16)
        rs_core[k, q] = send(pf.at[k, q, 1 - c], rf.at[k, q], rs_s.at[0, k, q], rs_r.at[0, k, q], core)
        rs_core[k, q].start()

    def stage_core(k, q):
        rs_core[k, q].wait_recv()
        theirs = pf[k, q, c, 1 - x].astype(jnp.float32) + rf[k, q, 1 - x].astype(jnp.float32)
        sf[k, q, 1 - x] = theirs.astype(jnp.bfloat16)
        rs_side[k, q] = send(sf.at[k, q, 1 - x], rxf.at[k, q], rs_s.at[1, k, q], rs_r.at[1, k, q], side)
        rs_side[k, q].start()
        ours = pf[k, q, c, x].astype(jnp.float32) + rf[k, q, x].astype(jnp.float32)
        sf[k, q, x] = ours.astype(jnp.bfloat16)

    def stage_side(k, q):
        rs_side[k, q].wait_recv()
        tf[k, q] = (sf[k, q, x].astype(jnp.float32) + rxf[k, q].astype(jnp.float32)).astype(jnp.bfloat16)
        if k > 0:
            to = {"fs": (f - k + n_fs) % n_fs}
            rs_z[k, q] = send(tf.at[k, q], rz.at[k, q], rs_s.at[2, k, q], rs_r.at[2, k, q], to)
            rs_z[k, q].start()

    own = [(0, q) for q in range(n_seq)]
    work = [(k, q) for k in ORDER for q in range(n_seq)]
    lag = len(own)
    every = own + work
    for i in range(len(work) + 6):
        if i < len(work):
            spread(*work[i])
        if i == 0:
            for cut in cuts:
                ffn_y[cut].wait_recv()
        if i < lag:
            block(*own[i])
        if 1 <= i <= len(work):
            pass_on(*work[i - 1])
        if 2 <= i < len(work) + 2:
            block(*work[i - 2])
        if 1 <= i <= len(every):
            stage_core(*every[i - 1])
        if 3 <= i < len(every) + 3:
            stage_side(*every[i - 3])

    fin_side, fin_core, fin_fwd = {}, {}, {}
    for q in range(n_seq):
        at = slice(q * SEQ_LEN, (q + 1) * SEQ_LEN)
        total = tf[0, q].astype(jnp.float32)
        for k in ORDER:
            rs_z[k, q].wait_recv()
            total = total + rz[k, q].astype(jnp.float32)
        bf[t, at] = total.astype(jnp.bfloat16)
        mine = bf.at[t, at]
        fin_side[q] = send(mine, mine, fin_s.at[0, q], fin_r.at[0, q], side)
        fin_side[q].start()
        fin_core[q] = send(mine, mine, fin_s.at[1, q], fin_r.at[1, q], core)
        fin_core[q].start()
    for q in range(n_seq):
        fin_side[q].wait_recv()
        theirs = bf.at[t_side, q * SEQ_LEN : (q + 1) * SEQ_LEN]
        fin_fwd[q] = send(theirs, theirs, fin_s.at[2, q], fin_r.at[2, q], core)
        fin_fwd[q].start()
    for q in range(n_seq):
        fin_core[q].wait_recv()
        fin_fwd[q].wait_recv()

    @pl.loop(0, rows // step_rows)
    def _(i):
        at = pl.ds(pl.multiple_of(i * step_rows, step_rows), step_rows)
        branch = jnp.concatenate([bf[j, at] for j in range(n_fs)], axis=1).astype(jnp.float32)
        out[at] = (middle[at].astype(jnp.float32) + norm_rows(branch, gain_ffn_post[...][None])).astype(jnp.bfloat16)

    groups = [mix_z, ffn_z, mix_y, ffn_y, mix_core, mix_side, mix_back]
    groups += [ag_z, ag_side, ag_core, ag_fwd, rs_core, rs_side, rs_z]
    groups += [fin_side, fin_core, fin_fwd]
    for group in groups:
        for copy in group.values():
            copy.wait_send()


def split_plan(
    n_fs,
    stream,
    mix_pre_gain,
    w_outer_gate,
    w_inner_gate,
    w_value,
    mix_taps,
    w_mix_out,
    mix_post_gain,
    ffn_pre_gain,
    w_linear,
    w_gated,
    ffn_taps,
    ffn_bias,
    w_down,
    ffn_post_gain,
):
    rows, model = stream.shape
    width, conv_w = w_value.shape
    units = w_linear.shape[1] // n_fs
    hid = -(-units // PACK) * PACK
    deep = -(-3 * hid // (2 * CHUNKS * PACK)) * 2 * CHUNKS * PACK
    cut = lambda rows_of: rows_of.reshape(n_fs, units, width)
    n_seq = rows // SEQ_LEN
    half = jnp.bfloat16
    vmem, dma = pltpu.VMEM, pltpu.SemaphoreType.DMA
    return pl.pallas_call(
        functools.partial(kernel, n_fs, conv_w, hid),
        out_shape=jax.ShapeDtypeStruct((rows, model), half),
        in_specs=[pl.BlockSpec(memory_space=vmem)] * 15,
        out_specs=pl.BlockSpec(memory_space=vmem),
        scratch_shapes=[
            vmem((n_fs, 8, hid), jnp.float32),
            vmem((n_fs, deep, width), half),
            vmem((n_fs, 4 * conv_w, width), half),
            vmem((n_fs, deep, width), half),
            vmem((n_fs, n_fs, rows, width), half),
            vmem((rows, model), half),
            vmem((rows, model), half),
            vmem((n_seq, 2, 2, SEQ_LEN, width), half),
            vmem((n_seq, 2, SEQ_LEN, width), half),
            vmem((n_seq, 2, SEQ_LEN, width), half),
            vmem((n_seq, 2, SEQ_LEN, width), half),
            vmem((n_seq, 2, 2, SEQ_LEN, width), half),
            vmem((n_fs, n_seq, 2, 2, SEQ_LEN, width), half),
            vmem((n_fs, n_seq, 2, SEQ_LEN, width), half),
            vmem((n_fs, n_seq, 2, SEQ_LEN, width), half),
            vmem((n_fs, n_seq, SEQ_LEN, width), half),
            vmem((n_fs, n_seq, SEQ_LEN, width), half),
            vmem((n_fs, n_seq, SEQ_LEN, width), half),
            vmem((n_fs, rows, width), half),
            dma((4, n_fs, CHUNKS)),
            dma((4, n_fs, CHUNKS)),
            dma((3, n_seq)),
            dma((3, n_seq)),
            dma((4, n_fs, n_seq)),
            dma((4, n_fs, n_seq)),
            dma((3, n_fs, n_seq)),
            dma((3, n_fs, n_seq)),
            dma((3, n_seq)),
            dma((3, n_seq)),
        ],
        compiler_params=pltpu.CompilerParams(
            collective_id=0, has_side_effects=True, vmem_limit_bytes=56 * 2**20
        ),
    )(
        stream,
        mix_pre_gain,
        mix_post_gain,
        ffn_pre_gain,
        ffn_post_gain,
        w_outer_gate.T,
        w_inner_gate.T,
        w_value.T,
        w_mix_out,
        mix_taps,
        cut(w_linear.T),
        cut(w_gated.T),
        cut(w_down),
        ffn_taps,
        ffn_bias,
    )


def on_device(rep, n_fs, n_tp, *arrays):
    stream, w_value, w_linear = arrays[0], arrays[4], arrays[9]
    same = n_fs == n_tp == 2 * rep == len(ORDER) + 1
    whole = w_value.shape[0] % 128 == 0 and w_value.shape[1] % (CHUNKS * PACK) == 0
    even = w_linear.shape[1] % n_fs == 0 and stream.shape[0] % SEQ_LEN == 0
    if same and rep == 2 and whole and even:
        return split_plan(n_fs, *arrays)
    return gather_plan(*arrays)


def solution(mesh):
    in_specs = (
        P(("rep", "fs"), None),
        P(),
        P("fs", "tp"),
        P("fs", "tp"),
        P("fs", "tp"),
        P(None, "tp"),
        P("tp", "fs"),
        P(),
        P(),
        P("fs", "tp"),
        P("fs", "tp"),
        P(None, "tp"),
        P("tp"),
        P("tp", "fs"),
        P(),
    )
    out_specs = P(("rep", "fs"), None)
    sizes = mesh.shape
    body = functools.partial(on_device, sizes["rep"], sizes["fs"], sizes["tp"])
    return jax.shard_map(
        body, mesh=mesh, in_specs=in_specs, out_specs=out_specs, check_vma=False
    )
```
